32 devices in a mesh: sp: 16 (over z, y, x), tp: 2 (over core).
Axes of the slice: x: 2, y: 2, z: 4, core: 2. Of those that a mesh axis runs over, the one named last changes fastest.
Arguments:
- skip_pathway: bfloat16 [2048, 2048], P('sp', 'tp'), may hold values from -6 to 6
- request_vectors: bfloat16 [2048, 1024], P('sp', 'tp'), may hold values from -6 to 6
- lookup_address_matrix: bfloat16 [2048, 1024], P('sp', 'tp'), may hold values from -6 to 6
- content_vectors: bfloat16 [2048, 1024], P('sp', 'tp'), may hold values from -6 to 6
- result_valve_matrix: bfloat16 [2048, 1024], P('sp', 'tp'), may hold values from -6 to 6
- shrink_raw_signal: float32 [2, 8, 2048], P(None, 'tp', 'sp'), may hold values from -3.1 to 3.6
- channel_shrink_speed: float32 [2, 8], P(None, 'tp'), may hold values from 2.4414063e-05 to 0.05
- insertion_raw_signal: float32 [2, 8, 2048], P(None, 'tp', 'sp'), may hold values from -8.5 to 2
- extra_shrink_spike: float32 [2, 8, 2048], P(None, 'tp', 'sp'), may hold values from -1.2 to 0
- channel_scaling_vector: float32 [128], replicated, may hold values from 0.1 to 1.9
- final_mapping_matrix: bfloat16 [1024, 2048], P(None, 'tp'), may hold values from -0.1875 to 0.1875
- mixer_scaling_vector: float32 [2048], replicated, may hold values from 0.1 to 1.9
- valve_matrix: bfloat16 [2048, 5120], P('sp', 'tp'), may hold values from -0.125 to 0.125
- widening_matrix: bfloat16 [2048, 5120], P('sp', 'tp'), may hold values from -0.125 to 0.125
- temporal_kernel_entries: float32 [3, 5120], P(None, 'tp'), may hold values from -3 to 3
- narrowing_matrix: bfloat16 [5120, 2048], P('tp', 'sp'), may hold values from -0.078125 to 0.078125
Outputs:
- result: bfloat16 [2048, 2048], P('sp', 'tp')
The draws below stay inside these ranges and needn't reach their ends.
All inputs are finite; a program needn't handle non-finite values.
Results may differ from the reference program's by a relative error of at most 0.009.
Values may be sent and summed in bfloat16 or wider, within the bound.
No kernel may reach another device: no remote copies, remote signals or barrier semaphores. Data moves between devices by JAX's collectives and lax.ppermute only.
A program may use at most 128 MiB of HBM per device.

```python
import math
import jax
import jax.numpy as jnp
from jax import lax

D = 2048
H = 8
DK = 128
DV = 128
FF = 5120
BLOCK = 64
TOK_DEV = 128
TOKENS = 2048
N_TP = 2


def head_kinds(key):
    share = 0.5
    return jax.random.bernoulli(jax.random.fold_in(key, 11), share, (2, H))


def draw_channel_shrink_speed(key, part):
    slow_head = head_kinds(key)
    slow_rate = jnp.exp(jax.random.uniform(jax.random.fold_in(key, 12), (2, H), jnp.float32, math.log(0.05), math.log(0.5))) / TOKENS
    fast_rate = jnp.exp(jax.random.uniform(jax.random.fold_in(key, 13), (2, H), jnp.float32, math.log(0.015), math.log(0.05)))
    return jnp.where(slow_head, slow_rate, fast_rate).astype(jnp.float32)


def draw_insertion_raw_signal(key, part):
    slow_head = head_kinds(key)
    base = jax.random.truncated_normal(jax.random.fold_in(key, 14), -2.0, 2.0, (2, H, TOKENS), jnp.float32)
    return jnp.where(slow_head[:, :, None], base - 6.5, base).astype(jnp.float32)


def draw_shrink_raw_signal(key, part):
    base = 0.7 * jax.random.truncated_normal(jax.random.fold_in(key, 15), -3.0, 3.0, (2, H, TOKENS), jnp.float32)
    offsets = jax.random.uniform(jax.random.fold_in(key, 16), (2, 1, TOKENS // TOK_DEV), jnp.float32, -1.0, 1.5)
    return (base + jnp.repeat(offsets, TOK_DEV, axis=2)).astype(jnp.float32)


def draw_extra_shrink_spike(key, part):
    places = jax.random.randint(jax.random.fold_in(key, 17), (2, H, 2), 0, TOKENS)
    amounts = jnp.log(jax.random.uniform(jax.random.fold_in(key, 18), (2, H, 2), jnp.float32, 0.55, 0.8))
    positions = jnp.arange(TOKENS, dtype=jnp.int32)
    hits = positions[None, None, None, :] == places[..., None]
    return jnp.sum(jnp.where(hits, amounts[..., None], 0.0), axis=2).astype(jnp.float32)


def shard_levels(stream_key, extent, pieces, low, high):
    level, own = 1.0, jax.random.fold_in(stream_key, 6)
    for axis_at, blocks in pieces:
        steps = jnp.exp(jax.random.uniform(jax.random.fold_in(own, axis_at), (blocks,), jnp.float32, low / len(pieces), high / len(pieces)))
        level = level * jnp.repeat(steps, extent[axis_at] // blocks).reshape([-1 if axis == axis_at else 1 for axis in range(len(extent))])
    return level


def scatter_about(stream_key, dims, scale, reach, cuts=(), kind=jnp.bfloat16):
    loudness = shard_levels(stream_key, dims, cuts, -0.22, 0.18) if cuts else 1.0
    entries = jax.random.normal(stream_key, dims, jnp.float32) * scale * loudness
    return jnp.minimum(jnp.maximum(entries, -reach), reach).astype(kind)


def setup_inputs(seed: int = 0) -> dict:
    arg_keys = jax.random.split(jax.random.key(seed), 17)
    return {
        "skip_pathway": scatter_about(arg_keys[0], (TOKENS, D), 1.0, 6.0, ((0, 16), (1, 2))),
        "request_vectors": scatter_about(arg_keys[1], (TOKENS, H * DK), 1.0, 6.0, ((0, 16), (1, 2))),
        "lookup_address_matrix": scatter_about(arg_keys[2], (TOKENS, H * DK), 1.0, 6.0, ((0, 16), (1, 2))),
        "content_vectors": scatter_about(arg_keys[3], (TOKENS, H * DV), 1.0, 6.0, ((0, 16), (1, 2))),
        "result_valve_matrix": scatter_about(arg_keys[4], (TOKENS, H * DV), 1.5, 6.0, ((0, 16), (1, 2))),
        "shrink_raw_signal": draw_shrink_raw_signal(jax.random.fold_in(arg_keys[16], 71), 0),
        "channel_shrink_speed": draw_channel_shrink_speed(jax.random.fold_in(arg_keys[16], 71), 0),
        "insertion_raw_signal": draw_insertion_raw_signal(jax.random.fold_in(arg_keys[16], 71), 0),
        "extra_shrink_spike": draw_extra_shrink_spike(jax.random.fold_in(arg_keys[16], 71), 0),
        "channel_scaling_vector": jnp.clip(1.0 + 0.18 * jax.random.normal(arg_keys[9], (DV,), jnp.float32), 0.1, 1.9),
        "final_mapping_matrix": scatter_about(arg_keys[10], (H * DV, D), (H * DV) ** -0.5, 0.1875, ((1, 2),)),
        "mixer_scaling_vector": jnp.clip(1.0 + 0.18 * jax.random.normal(arg_keys[11], (D,), jnp.float32), 0.1, 1.9),
        "valve_matrix": scatter_about(arg_keys[12], (D, FF), D ** -0.5, 0.125, ((0, 16), (1, 2))),
        "widening_matrix": scatter_about(arg_keys[13], (D, FF), D ** -0.5, 0.125, ((0, 16), (1, 2))),
        "temporal_kernel_entries": scatter_about(arg_keys[14], (3, FF), 0.5, 3.0, ((1, 2),), jnp.float32),
        "narrowing_matrix": scatter_about(arg_keys[15], (FF, D), FF ** -0.5, 0.078125, ((0, 2), (1, 16))),
    }


HIGHEST = lax.Precision.HIGHEST

def heads_of(matrix, head_size):
    return jnp.transpose(matrix.astype(jnp.float32).reshape(matrix.shape[0], -1, head_size), (1, 0, 2))

def unit_rows(vectors):
    return vectors * lax.rsqrt(lax.optimization_barrier(jnp.sum(vectors * vectors, axis=-1, keepdims=True)) + 1e-06)

def inverse_unit_lower(strict):
    width = strict.shape[-1]
    identity = jnp.eye(width, dtype=jnp.float32)
    powered = -strict
    result = identity + powered
    covered = 2
    while covered < width:
        powered = jnp.matmul(powered, powered, precision=HIGHEST)
        result = jnp.matmul(result, identity + powered, precision=HIGHEST)
        covered = covered * 2
    return result

def block_parts(queries, keys, values, shrink_exponent, beta, width):
    heads, length, key_size = queries.shape
    value_size = values.shape[-1]
    count = length // width
    queries = queries.reshape(heads, count, width, key_size)
    keys = keys.reshape(heads, count, width, key_size)
    values = values.reshape(heads, count, width, value_size)
    shrink_exponent = shrink_exponent.reshape(heads, count, width)
    beta = beta.reshape(heads, count, width)
    cumulative = jnp.cumsum(shrink_exponent, axis=-1)
    inside = jnp.tril(jnp.ones((width, width), dtype=bool))
    decay = jnp.exp(jnp.where(inside, cumulative[..., :, None] - cumulative[..., None, :], -jnp.inf))
    weighted = keys * beta[..., None]
    strict = jnp.tril(jnp.einsum('hnid,hnjd->hnij', weighted, keys, precision=HIGHEST) * decay, -1)
    inverse = inverse_unit_lower(strict)
    writes = jnp.matmul(inverse, values * beta[..., None], precision=HIGHEST)
    erases = jnp.matmul(inverse, weighted * jnp.exp(cumulative)[..., None], precision=HIGHEST)
    within = jnp.einsum('hnid,hnjd->hnij', queries, keys, precision=HIGHEST) * decay
    query_decayed = queries * jnp.exp(cumulative)[..., None]
    keys_decayed = keys * jnp.exp(cumulative[..., -1:] - cumulative)[..., None]
    block_decay = jnp.exp(cumulative[..., -1])
    return (query_decayed, keys_decayed, erases, writes, within, block_decay)

def run_blocks(parts, state):

    def advance(carry, block):
        query_decayed, keys_decayed, erases, writes, within, block_decay = block
        fresh = writes - jnp.matmul(erases, carry, precision=HIGHEST)
        output = jnp.matmul(query_decayed, carry, precision=HIGHEST) + jnp.matmul(within, fresh, precision=HIGHEST)
        carry = carry * block_decay[:, None, None] + jnp.matmul(jnp.swapaxes(keys_decayed, -1, -2), fresh, precision=HIGHEST)
        return (carry, output)
    blocks = tuple((jnp.moveaxis(item, 1, 0) for item in parts))
    final, outputs = lax.scan(advance, state, blocks)
    outputs = jnp.moveaxis(outputs, 0, 1)
    return outputs.reshape(outputs.shape[0], -1, outputs.shape[-1])

def gate_heads(mixture, result_valve_matrix, channel_scaling_vector):
    scaled = mixture * lax.rsqrt(lax.optimization_barrier(jnp.mean(mixture * mixture, axis=-1, keepdims=True)) + 1e-06) * channel_scaling_vector
    gated = scaled * jax.nn.silu(heads_of(result_valve_matrix, mixture.shape[-1]))
    return jnp.transpose(gated, (1, 0, 2)).reshape(gated.shape[1], -1).astype(jnp.bfloat16)

def rms_rows(rows, gain):
    widened = rows.astype(jnp.float32)
    return (widened * lax.rsqrt(lax.optimization_barrier(jnp.mean(widened * widened, axis=-1, keepdims=True)) + 1e-06) * gain).astype(jnp.bfloat16)

def reference(skip_pathway, request_vectors, lookup_address_matrix, content_vectors, result_valve_matrix, shrink_raw_signal, channel_shrink_speed, insertion_raw_signal, extra_shrink_spike, channel_scaling_vector, final_mapping_matrix, mixer_scaling_vector, valve_matrix, widening_matrix, temporal_kernel_entries, narrowing_matrix):
    queries = unit_rows(heads_of(request_vectors, DK)) * DK ** (-0.5)
    keys = unit_rows(heads_of(lookup_address_matrix, DK))
    values = heads_of(content_vectors, DV)
    shrink_exponent = -channel_shrink_speed[:, :, None] * jax.nn.softplus(shrink_raw_signal) + extra_shrink_spike
    beta = jax.nn.sigmoid(insertion_raw_signal)
    empty = jnp.zeros((H, DK, DV), jnp.float32)
    forward = run_blocks(block_parts(queries, keys, values, shrink_exponent[0], beta[0], BLOCK), empty)
    flipped = block_parts(jnp.flip(queries, 1), jnp.flip(keys, 1), jnp.flip(values, 1), jnp.flip(shrink_exponent[1], 1), jnp.flip(beta[1], 1), BLOCK)
    backward = jnp.flip(run_blocks(flipped, empty), 1)
    mixed = gate_heads(forward + backward, result_valve_matrix, channel_scaling_vector)
    projected = jnp.dot(mixed, final_mapping_matrix, preferred_element_type=jnp.float32)
    middle = (skip_pathway.astype(jnp.float32) + projected).astype(jnp.bfloat16)
    normed = rms_rows(middle, mixer_scaling_vector)
    gate = jnp.dot(normed, valve_matrix, preferred_element_type=jnp.float32).astype(jnp.bfloat16)
    up = jnp.dot(normed, widening_matrix, preferred_element_type=jnp.float32)
    padded = jnp.pad(gate, ((1, 1), (0, 0))).astype(jnp.float32)
    convolved = padded[:-2] * temporal_kernel_entries[0] + padded[1:-1] * temporal_kernel_entries[1] + padded[2:] * temporal_kernel_entries[2]
    hidden = (jax.nn.silu(convolved) * up).astype(jnp.bfloat16)
    group = FF // N_TP
    down = jnp.zeros((TOKENS, D), jnp.float32)
    for index in range(N_TP):
        partial_value = jnp.dot(hidden[:, index * group:(index + 1) * group], narrowing_matrix[index * group:(index + 1) * group], preferred_element_type=jnp.float32).astype(jnp.bfloat16)
        partial_value = lax.optimization_barrier(partial_value)
        down = down + partial_value.astype(jnp.float32)
    return (middle.astype(jnp.float32) + down).astype(jnp.bfloat16)
```

```python
import functools
import jax
import jax.numpy as jnp
from jax import lax
from jax.experimental import pallas as pl
from jax.experimental.pallas import tpu as pltpu
from jax.sharding import Mesh, PartitionSpec as P

DK = 128
EPS = 1e-06
F32 = jnp.float32
BF16 = jnp.bfloat16


def halves(x):
    high = x.astype(BF16)
    return high, (x - high.astype(F32)).astype(BF16)


def contract(a, b, da, db):
    return lax.dot_general(a, b, (((da,), (db,)), ((), ())), preferred_element_type=F32)


def dot(a, b):
    ah, al = halves(a)
    bh, bl = halves(b)
    return contract(ah, bh, 1, 0) + (contract(ah, bl, 1, 0) + contract(al, bh, 1, 0))


def dot_tn(a, b):
    return dot(jnp.transpose(a), b)


def dot_nt(a, b):
    return contract(a, b, 1, 1)


def inverse_unit_triangular(strict, row, col):
    width = strict.shape[0]
    identity = (row == col).astype(F32)
    size = 1
    inverse = identity
    while size < width:
        pair = (row // (2 * size) == col // (2 * size)) & (row // size != col // size)
        off = jnp.where(pair, strict, 0.0)
        if size == 1:
            inverse = inverse - off
        else:
            inverse = inverse - dot(inverse, dot(off, inverse))
        size *= 2
    return inverse


def delta_kernel(tokens_ref, scalars_ref, reach_ref, own_ref, maps_ref, *, width):
    length = tokens_ref.shape[0]
    count = length // width
    row = lax.broadcasted_iota(jnp.int32, (width, width), 0)
    col = lax.broadcasted_iota(jnp.int32, (width, width), 1)
    eye = row == col
    identity = eye.astype(F32)
    blocks = []
    for n in range(count):
        at = pl.ds(n * width, width)
        q = tokens_ref[at, 0:DK]
        k = tokens_ref[at, DK : 2 * DK]
        v = tokens_ref[at, 2 * DK : 3 * DK].astype(F32)
        qf = q.astype(F32)
        kf = k.astype(F32)
        kk = dot_nt(k, k)
        qk = dot_nt(q, k)
        diagonal = jnp.where(eye, kk, 0.0)
        key_col = lax.rsqrt(jnp.sum(kf * kf, axis=1, keepdims=True) + EPS)
        key_row = lax.rsqrt(jnp.sum(diagonal, axis=0, keepdims=True) + EPS)
        query_col = lax.rsqrt(jnp.sum(qf * qf, axis=1, keepdims=True) + EPS) * DK ** (-0.5)
        kk = kk * key_col * key_row
        qk = qk * query_col * key_row
        keys = kf * key_col
        queries = qf * query_col
        across = scalars_ref[:, at]
        down = jnp.transpose(across)
        pieces = []
        for d in range(2):
            inside = (col <= row) if d == 0 else (col >= row)
            strict_mask = inside & ~eye
            ld_row = across[d : d + 1]
            ld_col = down[:, d : d + 1]
            beta = down[:, 2 + d : 3 + d]
            cum_col = jnp.sum(jnp.where(inside, ld_row, 0.0), axis=1, keepdims=True)
            sooner = (row <= col) if d == 0 else (row >= col)
            cum_row = jnp.sum(jnp.where(sooner, ld_col, 0.0), axis=0, keepdims=True)
            total = jnp.sum(ld_row, axis=1, keepdims=True)
            decay = jnp.exp(jnp.where(inside, cum_col - cum_row, -1e30))
            strict = jnp.where(strict_mask, kk * decay * beta, 0.0)
            inverse = inverse_unit_triangular(strict, row, col)
            grown = jnp.exp(cum_col)
            rhs = jnp.concatenate([keys * (beta * grown), v * beta], axis=1)
            solved = dot(inverse, rhs)
            reading = dot(qk * decay, solved)
            keys_decayed = keys * jnp.exp(total - cum_col)
            carried = dot_tn(keys_decayed, solved)
            reach = queries * grown - reading[:, :DK]
            transition = identity * jnp.exp(total) - carried[:, :DK]
            pieces.append((reach, reading[:, DK:], transition, carried[:, DK:]))
        blocks.append(pieces)
    own = [None] * count
    for d in range(2):
        state = None
        order = range(count) if d == 0 else range(count - 1, -1, -1)
        for n in order:
            reach, local, transition, addition = blocks[n][d]
            if state is None:
                state = jnp.concatenate([transition, addition], axis=1)
            else:
                both = dot(jnp.concatenate([reach, transition], axis=0), state)
                reach = both[:width, :DK]
                local = local + both[:width, DK:]
                state = both[width:] + jnp.concatenate(
                    [jnp.zeros_like(addition), addition], axis=1
                )
            reach_ref[d, pl.ds(n * width, width)] = reach
            own[n] = local if own[n] is None else own[n] + local
        maps_ref[d] = state
    for n in range(count):
        own_ref[pl.ds(n * width, width)] = own[n]


def finish_kernel(place_ref, maps_ref, reach_ref, own_ref, valve_ref, gain_ref, mixed_ref):
    z = place_ref[0]
    planes = maps_ref.shape[0]
    empty = jnp.zeros((DK, own_ref.shape[1]), F32)

    def absorb(at, state):
        item = maps_ref[at]
        return dot(item[:, :DK], state) + item[:, DK:]

    ahead = lax.fori_loop(0, z, absorb, empty)
    behind = lax.fori_loop(
        0, planes - 1 - z, lambda i, state: absorb(planes - 1 - i, state), empty
    )
    o = own_ref[...] + dot(reach_ref[0], ahead) + dot(reach_ref[1], behind)
    scaled = o * lax.rsqrt(jnp.mean(o * o, axis=1, keepdims=True) + EPS) * gain_ref[...]
    valve = valve_ref[...].astype(F32)
    mixed_ref[...] = (scaled * (valve / (1.0 + jnp.exp(-valve)))).astype(BF16)


def vmem(count):
    return [pl.BlockSpec(memory_space=pltpu.VMEM)] * count


def delta_rule(tokens, scalars):
    length = tokens.shape[0]
    width = min(128, length)
    return pl.pallas_call(
        functools.partial(delta_kernel, width=width),
        out_shape=(
            jax.ShapeDtypeStruct((2, length, DK), F32),
            jax.ShapeDtypeStruct((length, DK), F32),
            jax.ShapeDtypeStruct((2, DK, 2 * DK), F32),
        ),
        in_specs=vmem(2),
        out_specs=tuple(vmem(3)),
        name="delta_rule",
    )(tokens, scalars)


def finish(place, maps, reach, own, valve, gain):
    return pl.pallas_call(
        finish_kernel,
        out_shape=jax.ShapeDtypeStruct(own.shape, BF16),
        in_specs=[pl.BlockSpec(memory_space=pltpu.SMEM)] + vmem(5),
        out_specs=pl.BlockSpec(memory_space=pltpu.VMEM),
        name="finish",
    )(place, maps, reach, own, valve, gain)


def exchange(slots, axis):
    return lax.all_to_all(slots, axis, split_axis=0, concat_axis=0, tiled=True)


def rms_rows(rows, gain):
    widened = rows.astype(F32)
    return (
        widened * lax.rsqrt(jnp.mean(widened * widened, axis=-1, keepdims=True) + EPS) * gain
    ).astype(BF16)


def to_columns(stack):
    return jnp.transpose(stack, (1, 0, 2)).reshape(stack.shape[1], -1)


def body(
    skip_pathway,
    request_vectors,
    lookup_address_matrix,
    content_vectors,
    result_valve_matrix,
    shrink_raw_signal,
    channel_shrink_speed,
    insertion_raw_signal,
    extra_shrink_spike,
    channel_scaling_vector,
    final_mapping_matrix,
    mixer_scaling_vector,
    valve_matrix,
    widening_matrix,
    temporal_kernel_entries,
    narrowing_matrix,
):
    group = lax.axis_size("p")
    planes = lax.axis_size("z")
    cores = lax.axis_size("tp")
    p = lax.axis_index("p")
    z = lax.axis_index("z")
    rows, features = skip_pathway.shape
    length = group * rows

    def spread(weight):
        parts = jnp.transpose(weight.reshape(rows_w(weight), group, -1), (1, 0, 2))
        return exchange(parts, "p").reshape(-1, parts.shape[-1])

    def rows_w(weight):
        return weight.shape[0]

    valve_rows = spread(valve_matrix)
    valve_full = lax.all_gather(valve_rows, "z", axis=0, tiled=True)
    widening_rows = spread(widening_matrix)
    widening_full = lax.all_gather(widening_rows, "z", axis=0, tiled=True)
    narrow_parts = narrowing_matrix.reshape(group, -1, narrowing_matrix.shape[1])
    narrow_cols = to_columns(exchange(narrow_parts, "p"))
    narrow_full = lax.all_gather(narrow_cols, "z", axis=1, tiled=True)

    packed = jnp.stack(
        [
            a.reshape(rows, group, DK)
            for a in (request_vectors, lookup_address_matrix, content_vectors, result_valve_matrix)
        ],
        axis=2,
    )
    packed = jnp.transpose(packed.reshape(rows, group, 4 * DK), (1, 0, 2))
    tokens = exchange(packed, "p").reshape(length, 4 * DK)
    log_decay = (
        -channel_shrink_speed[:, :, None] * jax.nn.softplus(shrink_raw_signal) + extra_shrink_spike
    )
    beta = jax.nn.sigmoid(insertion_raw_signal)
    scalars = jnp.concatenate([log_decay, beta, jnp.zeros_like(log_decay), jnp.zeros_like(beta)], axis=0)
    scalars = exchange(jnp.transpose(scalars, (1, 0, 2)), "p")
    scalars = to_columns(scalars)

    reach, own, maps = delta_rule(tokens, scalars)
    plane_ids = jnp.arange(planes).reshape(planes, 1, 1)
    outgoing = jnp.where(plane_ids > z, maps[0][None], maps[1][None])
    incoming = exchange(outgoing, "z")
    mixed = finish(
        z.reshape(1).astype(jnp.int32),
        incoming,
        reach,
        own,
        tokens[:, 3 * DK :],
        channel_scaling_vector.reshape(1, -1),
    )

    heads = to_columns(lax.all_gather(mixed, "p", axis=0))
    heads = exchange(jnp.broadcast_to(heads[None], (cores,) + heads.shape), "tp")
    projected = jnp.dot(
        to_columns(heads), final_mapping_matrix, preferred_element_type=F32
    )
    skip = exchange(jnp.broadcast_to(skip_pathway[None], (group, rows, features)), "p")
    middle = (skip.reshape(length, features).astype(F32) + projected).astype(BF16)
    full_rows = to_columns(exchange(jnp.broadcast_to(middle[None], (cores,) + middle.shape), "tp"))
    normed = rms_rows(full_rows, mixer_scaling_vector)

    gate = jnp.dot(normed, valve_full, preferred_element_type=F32).astype(BF16)
    up = jnp.dot(normed, widening_full, preferred_element_type=F32)
    size = planes
    before = lax.ppermute(gate[-1:], "z", [(i, i + 1) for i in range(size - 1)])
    after = lax.ppermute(gate[:1], "z", [(i + 1, i) for i in range(size - 1)])
    padded = jnp.concatenate([before, gate, after], axis=0).astype(F32)
    units = gate.shape[1]
    taps = lax.dynamic_slice_in_dim(temporal_kernel_entries, p * units, units, axis=1)
    convolved = padded[:-2] * taps[0] + padded[1:-1] * taps[1] + padded[2:] * taps[2]
    hidden = (jax.nn.silu(convolved) * up).astype(BF16)
    terms = jnp.dot(hidden, narrow_full, preferred_element_type=F32).astype(BF16)
    terms = jnp.transpose(terms.reshape(group, rows, cores, features), (0, 2, 1, 3))
    terms = exchange(terms.reshape(group * cores, rows, features), ("p", "tp"))
    down = jnp.sum(terms.astype(F32), axis=0)
    mine = lax.dynamic_slice_in_dim(middle, p * rows, rows, axis=0)
    return (mine.astype(F32) + down).astype(BF16)


def solution(mesh):
    def layer(*args):
        cores = mesh.shape["tp"]
        group = args[5].shape[1] // cores
        split = Mesh(mesh.devices.reshape(-1, group, cores), ("z", "p", "tp"))
        sp = ("z", "p")
        return jax.shard_map(
            body,
            mesh=split,
            in_specs=(
                P(sp, "tp"),
                P(sp, "tp"),
                P(sp, "tp"),
                P(sp, "tp"),
                P(sp, "tp"),
                P(None, "tp", sp),
                P(None, "tp"),
                P(None, "tp", sp),
                P(None, "tp", sp),
                P(),
                P(None, "tp"),
                P(),
                P(sp, "tp"),
                P(sp, "tp"),
                P(None, "tp"),
                P("tp", sp),
            ),
            out_specs=P(sp, "tp"),
            check_vma=False,
        )(*args)

    return layer
```

```python
import functools
import jax
import jax.numpy as jnp
from jax import lax
from jax.experimental import pallas as pl
from jax.experimental.pallas import tpu as pltpu
from jax.sharding import Mesh, PartitionSpec as P

DK = 128
EPS = 1e-06
F32 = jnp.float32
BF16 = jnp.bfloat16


def halves(x):
    high = x.astype(BF16)
    return high, (x - high.astype(F32)).astype(BF16)


def contract(a, b, da, db):
    return lax.dot_general(a, b, (((da,), (db,)), ((), ())), preferred_element_type=F32)


def dot(a, b):
    ah, al = halves(a)
    bh, bl = halves(b)
    return contract(ah, bh, 1, 0) + (contract(ah, bl, 1, 0) + contract(al, bh, 1, 0))


def dot_tn(a, b):
    return dot(jnp.transpose(a), b)


def dot_nt(a, b):
    return contract(a, b, 1, 1)


def inverse_unit_triangular(strict, row, col):
    width = strict.shape[0]
    identity = (row == col).astype(F32)
    size = 1
    inverse = identity
    while size < width:
        pair = (row // (2 * size) == col // (2 * size)) & (row // size != col // size)
        off = jnp.where(pair, strict, 0.0)
        if size == 1:
            inverse = inverse - off
        else:
            inverse = inverse - dot(inverse, dot(off, inverse))
        size *= 2
    return inverse


def delta_kernel(tokens_ref, scalars_ref, reach_ref, own_ref, maps_ref, *, width):
    length = tokens_ref.shape[0]
    count = length // width
    row = lax.broadcasted_iota(jnp.int32, (width, width), 0)
    col = lax.broadcasted_iota(jnp.int32, (width, width), 1)
    eye = row == col
    identity = eye.astype(F32)
    blocks = []
    for n in range(count):
        at = pl.ds(n * width, width)
        q = tokens_ref[at, 0:DK]
        k = tokens_ref[at, DK : 2 * DK]
        v = tokens_ref[at, 2 * DK : 3 * DK].astype(F32)
        qf = q.astype(F32)
        kf = k.astype(F32)
        kk = dot_nt(k, k)
        qk = dot_nt(q, k)
        diagonal = jnp.where(eye, kk, 0.0)
        key_col = lax.rsqrt(jnp.sum(kf * kf, axis=1, keepdims=True) + EPS)
        key_row = lax.rsqrt(jnp.sum(diagonal, axis=0, keepdims=True) + EPS)
        query_col = lax.rsqrt(jnp.sum(qf * qf, axis=1, keepdims=True) + EPS) * DK ** (-0.5)
        kk = kk * key_col * key_row
        qk = qk * query_col * key_row
        keys = kf * key_col
        queries = qf * query_col
        across = scalars_ref[:, at]
        down = jnp.transpose(across)
        pieces = []
        for d in range(2):
            inside = (col <= row) if d == 0 else (col >= row)
            strict_mask = inside & ~eye
            ld_row = across[d : d + 1]
            ld_col = down[:, d : d + 1]
            beta = down[:, 2 + d : 3 + d]
            cum_col = jnp.sum(jnp.where(inside, ld_row, 0.0), axis=1, keepdims=True)
            sooner = (row <= col) if d == 0 else (row >= col)
            cum_row = jnp.sum(jnp.where(sooner, ld_col, 0.0), axis=0, keepdims=True)
            total = jnp.sum(ld_row, axis=1, keepdims=True)
            decay = jnp.exp(jnp.where(inside, cum_col - cum_row, -1e30))
            strict = jnp.where(strict_mask, kk * decay * beta, 0.0)
            inverse = inverse_unit_triangular(strict, row, col)
            grown = jnp.exp(cum_col)
            rhs = jnp.concatenate([keys * (beta * grown), v * beta], axis=1)
            solved = dot(inverse, rhs)
            reading = dot(qk * decay, solved)
            keys_decayed = keys * jnp.exp(total - cum_col)
            carried = dot_tn(keys_decayed, solved)
            reach = queries * grown - reading[:, :DK]
            transition = identity * jnp.exp(total) - carried[:, :DK]
            pieces.append((reach, reading[:, DK:], transition, carried[:, DK:]))
        blocks.append(pieces)
    own = [None] * count
    for d in range(2):
        state = None
        order = range(count) if d == 0 else range(count - 1, -1, -1)
        for n in order:
            reach, local, transition, addition = blocks[n][d]
            if state is None:
                state = jnp.concatenate([transition, addition], axis=1)
            else:
                both = dot(jnp.concatenate([reach, transition], axis=0), state)
                reach = both[:width, :DK]
                local = local + both[:width, DK:]
                state = both[width:] + jnp.concatenate(
                    [jnp.zeros_like(addition), addition], axis=1
                )
            reach_ref[d, pl.ds(n * width, width)] = reach
            own[n] = local if own[n] is None else own[n] + local
        maps_ref[d] = state
    for n in range(count):
        own_ref[pl.ds(n * width, width)] = own[n]


def finish_kernel(place_ref, maps_ref, reach_ref, own_ref, valve_ref, gain_ref, mixed_ref):
    z = place_ref[0]
    planes = maps_ref.shape[0]
    empty = jnp.zeros((DK, own_ref.shape[1]), F32)

    def absorb(at, state):
        item = maps_ref[at]
        return dot(item[:, :DK], state) + item[:, DK:]

    ahead = lax.fori_loop(0, z, absorb, empty)
    behind = lax.fori_loop(
        0, planes - 1 - z, lambda i, state: absorb(planes - 1 - i, state), empty
    )
    o = own_ref[...] + dot(reach_ref[0], ahead) + dot(reach_ref[1], behind)
    scaled = o * lax.rsqrt(jnp.mean(o * o, axis=1, keepdims=True) + EPS) * gain_ref[...]
    valve = valve_ref[...].astype(F32)
    mixed_ref[...] = (scaled * (valve / (1.0 + jnp.exp(-valve)))).astype(BF16)


def vmem(count):
    return [pl.BlockSpec(memory_space=pltpu.VMEM)] * count


def delta_rule(tokens, scalars):
    length = tokens.shape[0]
    width = min(128, length)
    return pl.pallas_call(
        functools.partial(delta_kernel, width=width),
        out_shape=(
            jax.ShapeDtypeStruct((2, length, DK), F32),
            jax.ShapeDtypeStruct((length, DK), F32),
            jax.ShapeDtypeStruct((2, DK, 2 * DK), F32),
        ),
        in_specs=vmem(2),
        out_specs=tuple(vmem(3)),
        name="delta_rule",
    )(tokens, scalars)


def finish(place, maps, reach, own, valve, gain):
    return pl.pallas_call(
        finish_kernel,
        out_shape=jax.ShapeDtypeStruct(own.shape, BF16),
        in_specs=[pl.BlockSpec(memory_space=pltpu.SMEM)] + vmem(5),
        out_specs=pl.BlockSpec(memory_space=pltpu.VMEM),
        name="finish",
    )(place, maps, reach, own, valve, gain)


def copy_kernel(*refs, moves, sources):
    inputs, output, semaphores = refs[:sources], refs[sources], refs[sources + 1]
    copies = []
    for index, (source, take, put) in enumerate(moves):
        copies.append(
            pltpu.make_async_copy(
                inputs[source].at[take], output.at[put], semaphores.at[index]
            )
        )
    for copy in copies:
        copy.start()
    for copy in copies:
        copy.wait()


def rearrange(arrays, shape, moves, name):
    count = len(arrays)
    return pl.pallas_call(
        functools.partial(copy_kernel, moves=tuple(moves), sources=count),
        out_shape=jax.ShapeDtypeStruct(shape, arrays[0].dtype),
        in_specs=[pl.BlockSpec(memory_space=pl.ANY)] * count,
        out_specs=pl.BlockSpec(memory_space=pl.ANY),
        scratch_shapes=[pltpu.SemaphoreType.DMA((len(moves),))],
        name=name,
    )(*arrays)


def span(index, size):
    return pl.ds(index * size, size)


ALL = slice(None)


def down_kernel(hidden_ref, weight_ref, out_ref):
    out_ref[0] = jnp.dot(
        hidden_ref[...], weight_ref[...], preferred_element_type=F32
    ).astype(BF16)


def down_product(hidden, weight, cores):
    length, units = hidden.shape
    features = weight.shape[1] // cores
    tile = min(512, features)
    steps = features // tile
    return pl.pallas_call(
        down_kernel,
        grid=(cores, steps),
        out_shape=jax.ShapeDtypeStruct((cores, length, features), BF16),
        in_specs=[
            pl.BlockSpec((length, units), lambda c, n: (0, 0)),
            pl.BlockSpec((units, tile), lambda c, n: (0, c * steps + n)),
        ],
        out_specs=pl.BlockSpec((1, length, tile), lambda c, n: (c, 0, n)),
        name="down",
    )(hidden, weight)


def exchange(slots, axis):
    return lax.all_to_all(slots, axis, split_axis=0, concat_axis=0, tiled=True)


def rms_rows(rows, gain):
    widened = rows.astype(F32)
    return (
        widened * lax.rsqrt(jnp.mean(widened * widened, axis=-1, keepdims=True) + EPS) * gain
    ).astype(BF16)


def to_columns(stack):
    return jnp.transpose(stack, (1, 0, 2)).reshape(stack.shape[1], -1)


def body(
    skip_pathway,
    request_vectors,
    lookup_address_matrix,
    content_vectors,
    result_valve_matrix,
    shrink_raw_signal,
    channel_shrink_speed,
    insertion_raw_signal,
    extra_shrink_spike,
    channel_scaling_vector,
    final_mapping_matrix,
    mixer_scaling_vector,
    valve_matrix,
    widening_matrix,
    temporal_kernel_entries,
    narrowing_matrix,
):
    group = lax.axis_size("p")
    planes = lax.axis_size("z")
    cores = lax.axis_size("tp")
    p = lax.axis_index("p")
    z = lax.axis_index("z")
    rows, features = skip_pathway.shape
    length = group * rows

    depth = valve_matrix.shape[0]
    units = valve_matrix.shape[1] // group
    moves = [
        (w, (ALL, span(j, units)), (j, w)) for j in range(group) for w in range(2)
    ]
    pair = rearrange(
        (valve_matrix, widening_matrix), (group, 2, depth, units), moves, "pack_pair"
    )
    pair = exchange(pair, "p")
    moves = [(0, (j, w), (w, j)) for j in range(group) for w in range(2)]
    pair = rearrange((pair,), (2, group, depth, units), moves, "place_pair")
    pair = pair.reshape(2, group * depth, units)
    pair = lax.all_gather(pair, "z", axis=1, tiled=True)
    width = narrowing_matrix.shape[1]
    narrow = exchange(narrowing_matrix.reshape(group, units, width), "p")
    if width % 128 == 0:
        moves = [(0, (j,), (ALL, span(j, width))) for j in range(group)]
        narrow = rearrange((narrow,), (units, group * width), moves, "place_narrow")
    else:
        narrow = to_columns(narrow)
    narrow_full = lax.all_gather(narrow, "z", axis=1, tiled=True)

    moves = [
        (a, (ALL, span(j, DK)), (j, ALL, span(a, DK))) for j in range(group) for a in range(4)
    ]
    packed = rearrange(
        (request_vectors, lookup_address_matrix, content_vectors, result_valve_matrix),
        (group, rows, 4 * DK),
        moves,
        "pack_tokens",
    )
    tokens = exchange(packed, "p").reshape(length, 4 * DK)
    log_decay = (
        -channel_shrink_speed[:, :, None] * jax.nn.softplus(shrink_raw_signal) + extra_shrink_spike
    )
    beta = jax.nn.sigmoid(insertion_raw_signal)
    scalars = jnp.concatenate([log_decay, beta, jnp.zeros_like(log_decay), jnp.zeros_like(beta)], axis=0)
    scalars = exchange(jnp.transpose(scalars, (1, 0, 2)), "p")
    scalars = to_columns(scalars)

    reach, own, maps = delta_rule(tokens, scalars)
    plane_ids = jnp.arange(planes).reshape(planes, 1, 1)
    outgoing = jnp.where(plane_ids > z, maps[0][None], maps[1][None])
    incoming = exchange(outgoing, "z")
    mixed = finish(
        z.reshape(1).astype(jnp.int32),
        incoming,
        reach,
        own,
        tokens[:, 3 * DK :],
        channel_scaling_vector.reshape(1, -1),
    )

    heads = to_columns(lax.all_gather(mixed, "p", axis=0))
    heads = exchange(jnp.broadcast_to(heads[None], (cores,) + heads.shape), "tp")
    projected = jnp.dot(
        to_columns(heads), final_mapping_matrix, preferred_element_type=F32
    )
    skip = exchange(jnp.broadcast_to(skip_pathway[None], (group, rows, features)), "p")
    middle = (skip.reshape(length, features).astype(F32) + projected).astype(BF16)
    full_rows = to_columns(exchange(jnp.broadcast_to(middle[None], (cores,) + middle.shape), "tp"))
    normed = rms_rows(full_rows, mixer_scaling_vector)

    gate = jnp.dot(normed, pair[0], preferred_element_type=F32).astype(BF16)
    up = jnp.dot(normed, pair[1], preferred_element_type=F32)
    before = lax.ppermute(gate[-1:], "z", [(i, i + 1) for i in range(planes - 1)])
    after = lax.ppermute(gate[:1], "z", [(i + 1, i) for i in range(planes - 1)])
    padded = jnp.concatenate([before, gate, after], axis=0).astype(F32)
    taps = lax.dynamic_slice_in_dim(temporal_kernel_entries, p * units, units, axis=1)
    convolved = padded[:-2] * taps[0] + padded[1:-1] * taps[1] + padded[2:] * taps[2]
    hidden = (jax.nn.silu(convolved) * up).astype(BF16)
    terms = down_product(hidden, narrow_full, cores)
    terms = jnp.sum(exchange(terms, "tp").astype(F32), axis=0).astype(BF16)
    terms = exchange(terms.reshape(group, rows, features), "p")
    down = jnp.sum(terms.astype(F32), axis=0)
    mine = lax.dynamic_slice_in_dim(middle, p * rows, rows, axis=0)
    return (mine.astype(F32) + down).astype(BF16)


def solution(mesh):
    def layer(*args):
        cores = mesh.shape["tp"]
        group = args[5].shape[1] // cores
        split = Mesh(mesh.devices.reshape(-1, group, cores), ("z", "p", "tp"))
        sp = ("z", "p")
        return jax.shard_map(
            body,
            mesh=split,
            in_specs=(
                P(sp, "tp"),
                P(sp, "tp"),
                P(sp, "tp"),
                P(sp, "tp"),
                P(sp, "tp"),
                P(None, "tp", sp),
                P(None, "tp"),
                P(None, "tp", sp),
                P(None, "tp", sp),
                P(),
                P(None, "tp"),
                P(),
                P(sp, "tp"),
                P(sp, "tp"),
                P(None, "tp"),
                P("tp", sp),
            ),
            out_specs=P(sp, "tp"),
            check_vma=False,
        )(*args)

    return layer
```

```python
import functools
import jax
import jax.numpy as jnp
from jax import lax
from jax.experimental import pallas as pl
from jax.experimental.pallas import tpu as pltpu
from jax.sharding import Mesh, PartitionSpec as P

DK = 128
EPS = 1e-06
F32 = jnp.float32
BF16 = jnp.bfloat16


def halves(x):
    high = x.astype(BF16)
    return high, (x - high.astype(F32)).astype(BF16)


def contract(a, b, da, db):
    return lax.dot_general(a, b, (((da,), (db,)), ((), ())), preferred_element_type=F32)


def dot(a, b):
    ah, al = halves(a)
    bh, bl = halves(b)
    return contract(ah, bh, 1, 0) + (contract(ah, bl, 1, 0) + contract(al, bh, 1, 0))


def dot_tn(a, b):
    return dot(jnp.transpose(a), b)


def dot_nt(a, b):
    return contract(a, b, 1, 1)


def inverse_unit_triangular(strict, row, col):
    width = strict.shape[0]
    identity = (row == col).astype(F32)
    size = 1
    inverse = identity
    while size < width:
        pair = (row // (2 * size) == col // (2 * size)) & (row // size != col // size)
        off = jnp.where(pair, strict, 0.0)
        if size == 1:
            inverse = inverse - off
        else:
            inverse = inverse - dot(inverse, dot(off, inverse))
        size *= 2
    return inverse


def delta_kernel(tokens_ref, scalars_ref, reach_ref, own_ref, maps_ref, *, width):
    length = tokens_ref.shape[0]
    count = length // width
    row = lax.broadcasted_iota(jnp.int32, (width, width), 0)
    col = lax.broadcasted_iota(jnp.int32, (width, width), 1)
    eye = row == col
    identity = eye.astype(F32)
    blocks = []
    for n in range(count):
        at = pl.ds(n * width, width)
        q = tokens_ref[at, 0:DK]
        k = tokens_ref[at, DK : 2 * DK]
        v = tokens_ref[at, 2 * DK : 3 * DK].astype(F32)
        qf = q.astype(F32)
        kf = k.astype(F32)
        kk = dot_nt(k, k)
        qk = dot_nt(q, k)
        diagonal = jnp.where(eye, kk, 0.0)
        key_col = lax.rsqrt(jnp.sum(kf * kf, axis=1, keepdims=True) + EPS)
        key_row = lax.rsqrt(jnp.sum(diagonal, axis=0, keepdims=True) + EPS)
        query_col = lax.rsqrt(jnp.sum(qf * qf, axis=1, keepdims=True) + EPS) * DK ** (-0.5)
        kk = kk * key_col * key_row
        qk = qk * query_col * key_row
        keys = kf * key_col
        queries = qf * query_col
        across = scalars_ref[:, at]
        down = jnp.transpose(across)
        pieces = []
        for d in range(2):
            inside = (col <= row) if d == 0 else (col >= row)
            strict_mask = inside & ~eye
            ld_row = across[d : d + 1]
            ld_col = down[:, d : d + 1]
            beta = down[:, 2 + d : 3 + d]
            cum_col = jnp.sum(jnp.where(inside, ld_row, 0.0), axis=1, keepdims=True)
            sooner = (row <= col) if d == 0 else (row >= col)
            cum_row = jnp.sum(jnp.where(sooner, ld_col, 0.0), axis=0, keepdims=True)
            total = jnp.sum(ld_row, axis=1, keepdims=True)
            decay = jnp.exp(jnp.where(inside, cum_col - cum_row, -1e30))
            strict = jnp.where(strict_mask, kk * decay * beta, 0.0)
            inverse = inverse_unit_triangular(strict, row, col)
            grown = jnp.exp(cum_col)
            rhs = jnp.concatenate([keys * (beta * grown), v * beta], axis=1)
            solved = dot(inverse, rhs)
            reading = dot(qk * decay, solved)
            keys_decayed = keys * jnp.exp(total - cum_col)
            carried = dot_tn(keys_decayed, solved)
            reach = queries * grown - reading[:, :DK]
            transition = identity * jnp.exp(total) - carried[:, :DK]
            pieces.append((reach, reading[:, DK:], transition, carried[:, DK:]))
        blocks.append(pieces)
    own = [None] * count
    for d in range(2):
        state = None
        order = range(count) if d == 0 else range(count - 1, -1, -1)
        for n in order:
            reach, local, transition, addition = blocks[n][d]
            if state is None:
                state = jnp.concatenate([transition, addition], axis=1)
            else:
                both = dot(jnp.concatenate([reach, transition], axis=0), state)
                reach = both[:width, :DK]
                local = local + both[:width, DK:]
                state = both[width:] + jnp.concatenate(
                    [jnp.zeros_like(addition), addition], axis=1
                )
            reach_ref[d, pl.ds(n * width, width)] = reach
            own[n] = local if own[n] is None else own[n] + local
        maps_ref[d] = state
    for n in range(count):
        own_ref[pl.ds(n * width, width)] = own[n]


def finish_kernel(place_ref, maps_ref, reach_ref, own_ref, valve_ref, gain_ref, mixed_ref):
    z = place_ref[0]
    planes = maps_ref.shape[0]
    empty = jnp.zeros((DK, own_ref.shape[1]), F32)

    def absorb(at, state):
        item = maps_ref[at]
        return dot(item[:, :DK], state) + item[:, DK:]

    ahead = lax.fori_loop(0, z, absorb, empty)
    behind = lax.fori_loop(
        0, planes - 1 - z, lambda i, state: absorb(planes - 1 - i, state), empty
    )
    o = own_ref[...] + dot(reach_ref[0], ahead) + dot(reach_ref[1], behind)
    scaled = o * lax.rsqrt(jnp.mean(o * o, axis=1, keepdims=True) + EPS) * gain_ref[...]
    valve = valve_ref[...].astype(F32)
    mixed_ref[...] = (scaled * (valve / (1.0 + jnp.exp(-valve)))).astype(BF16)


def vmem(count):
    return [pl.BlockSpec(memory_space=pltpu.VMEM)] * count


def delta_rule(tokens, scalars):
    length = tokens.shape[0]
    width = min(128, length)
    return pl.pallas_call(
        functools.partial(delta_kernel, width=width),
        out_shape=(
            jax.ShapeDtypeStruct((2, length, DK), F32),
            jax.ShapeDtypeStruct((length, DK), F32),
            jax.ShapeDtypeStruct((2, DK, 2 * DK), F32),
        ),
        in_specs=vmem(2),
        out_specs=tuple(vmem(3)),
        name="delta_rule",
    )(tokens, scalars)


def finish(place, maps, reach, own, valve, gain):
    return pl.pallas_call(
        finish_kernel,
        out_shape=jax.ShapeDtypeStruct(own.shape, BF16),
        in_specs=[pl.BlockSpec(memory_space=pltpu.SMEM)] + vmem(5),
        out_specs=pl.BlockSpec(memory_space=pltpu.VMEM),
        name="finish",
    )(place, maps, reach, own, valve, gain)


def copy_kernel(*refs, moves, sources):
    output = refs[sources]
    for source, take, put in moves:
        output[put] = refs[source][take]


def rearrange(arrays, shape, moves, name):
    count = len(arrays)
    return pl.pallas_call(
        functools.partial(copy_kernel, moves=tuple(moves), sources=count),
        out_shape=jax.ShapeDtypeStruct(shape, arrays[0].dtype),
        in_specs=vmem(count),
        out_specs=pl.BlockSpec(memory_space=pltpu.VMEM),
        name=name,
    )(*arrays)


def span(index, size):
    return pl.ds(index * size, size)


ALL = slice(None)


def down_kernel(hidden_ref, weight_ref, out_ref):
    out_ref[0] = jnp.dot(
        hidden_ref[...], weight_ref[...], preferred_element_type=F32
    ).astype(BF16)


def down_product(hidden, weight, cores):
    length, units = hidden.shape
    features = weight.shape[1] // cores
    tile = min(512, features)
    steps = features // tile
    return pl.pallas_call(
        down_kernel,
        grid=(cores, steps),
        out_shape=jax.ShapeDtypeStruct((cores, length, features), BF16),
        in_specs=[
            pl.BlockSpec((length, units), lambda c, n: (0, 0)),
            pl.BlockSpec((units, tile), lambda c, n: (0, c * steps + n)),
        ],
        out_specs=pl.BlockSpec((1, length, tile), lambda c, n: (c, 0, n)),
        name="down",
    )(hidden, weight)


def exchange(slots, axis):
    return lax.all_to_all(slots, axis, split_axis=0, concat_axis=0, tiled=True)


def rms_rows(rows, gain):
    widened = rows.astype(F32)
    return (
        widened * lax.rsqrt(jnp.mean(widened * widened, axis=-1, keepdims=True) + EPS) * gain
    ).astype(BF16)


def to_columns(stack):
    return jnp.transpose(stack, (1, 0, 2)).reshape(stack.shape[1], -1)


def body(
    skip_pathway,
    request_vectors,
    lookup_address_matrix,
    content_vectors,
    result_valve_matrix,
    shrink_raw_signal,
    channel_shrink_speed,
    insertion_raw_signal,
    extra_shrink_spike,
    channel_scaling_vector,
    final_mapping_matrix,
    mixer_scaling_vector,
    valve_matrix,
    widening_matrix,
    temporal_kernel_entries,
    narrowing_matrix,
):
    group = lax.axis_size("p")
    planes = lax.axis_size("z")
    cores = lax.axis_size("tp")
    p = lax.axis_index("p")
    z = lax.axis_index("z")
    rows, features = skip_pathway.shape
    length = group * rows

    depth = valve_matrix.shape[0]
    units = valve_matrix.shape[1] // group
    moves = [
        (w, (ALL, span(j, units)), (j, w)) for j in range(group) for w in range(2)
    ]
    pair = rearrange(
        (valve_matrix, widening_matrix), (group, 2, depth, units), moves, "pack_pair"
    )
    pair = exchange(pair, "p")
    moves = [(0, (j, w), (w, j)) for j in range(group) for w in range(2)]
    pair = rearrange((pair,), (2, group, depth, units), moves, "place_pair")
    pair = pair.reshape(2, group * depth, units)
    pair = lax.all_gather(pair, "z", axis=1, tiled=True)
    width = narrowing_matrix.shape[1]
    narrow = exchange(narrowing_matrix.reshape(group, units, width), "p")
    if width % 128 == 0:
        moves = [(0, (j,), (ALL, span(j, width))) for j in range(group)]
        narrow = rearrange((narrow,), (units, group * width), moves, "place_narrow")
    else:
        narrow = to_columns(narrow)
    narrow_full = lax.all_gather(narrow, "z", axis=1, tiled=True)

    moves = [
        (a, (ALL, span(j, DK)), (j, ALL, span(a, DK))) for j in range(group) for a in range(4)
    ]
    packed = rearrange(
        (request_vectors, lookup_address_matrix, content_vectors, result_valve_matrix),
        (group, rows, 4 * DK),
        moves,
        "pack_tokens",
    )
    tokens = exchange(packed, "p").reshape(length, 4 * DK)
    log_decay = (
        -channel_shrink_speed[:, :, None] * jax.nn.softplus(shrink_raw_signal) + extra_shrink_spike
    )
    beta = jax.nn.sigmoid(insertion_raw_signal)
    scalars = jnp.concatenate([log_decay, beta, jnp.zeros_like(log_decay), jnp.zeros_like(beta)], axis=0)
    scalars = exchange(jnp.transpose(scalars, (1, 0, 2)), "p")
    scalars = to_columns(scalars)

    reach, own, maps = delta_rule(tokens, scalars)
    plane_ids = jnp.arange(planes).reshape(planes, 1, 1)
    outgoing = jnp.where(plane_ids > z, maps[0][None], maps[1][None])
    incoming = exchange(outgoing, "z")
    mixed = finish(
        z.reshape(1).astype(jnp.int32),
        incoming,
        reach,
        own,
        tokens[:, 3 * DK :],
        channel_scaling_vector.reshape(1, -1),
    )

    heads = to_columns(lax.all_gather(mixed, "p", axis=0))
    heads = exchange(jnp.broadcast_to(heads[None], (cores,) + heads.shape), "tp")
    projected = jnp.dot(
        to_columns(heads), final_mapping_matrix, preferred_element_type=F32
    )
    skip = exchange(jnp.broadcast_to(skip_pathway[None], (group, rows, features)), "p")
    middle = (skip.reshape(length, features).astype(F32) + projected).astype(BF16)
    full_rows = to_columns(exchange(jnp.broadcast_to(middle[None], (cores,) + middle.shape), "tp"))
    normed = rms_rows(full_rows, mixer_scaling_vector)

    gate = jnp.dot(normed, pair[0], preferred_element_type=F32).astype(BF16)
    up = jnp.dot(normed, pair[1], preferred_element_type=F32)
    before = lax.ppermute(gate[-1:], "z", [(i, i + 1) for i in range(planes - 1)])
    after = lax.ppermute(gate[:1], "z", [(i + 1, i) for i in range(planes - 1)])
    padded = jnp.concatenate([before, gate, after], axis=0).astype(F32)
    taps = lax.dynamic_slice_in_dim(temporal_kernel_entries, p * units, units, axis=1)
    convolved = padded[:-2] * taps[0] + padded[1:-1] * taps[1] + padded[2:] * taps[2]
    hidden = (jax.nn.silu(convolved) * up).astype(BF16)
    terms = down_product(hidden, narrow_full, cores)
    terms = jnp.sum(exchange(terms, "tp").astype(F32), axis=0).astype(BF16)
    terms = exchange(terms.reshape(group, rows, features), "p")
    down = jnp.sum(terms.astype(F32), axis=0)
    mine = lax.dynamic_slice_in_dim(middle, p * rows, rows, axis=0)
    return (mine.astype(F32) + down).astype(BF16)


def solution(mesh):
    def layer(*args):
        cores = mesh.shape["tp"]
        group = args[5].shape[1] // cores
        split = Mesh(mesh.devices.reshape(-1, group, cores), ("z", "p", "tp"))
        sp = ("z", "p")
        return jax.shard_map(
            body,
            mesh=split,
            in_specs=(
                P(sp, "tp"),
                P(sp, "tp"),
                P(sp, "tp"),
                P(sp, "tp"),
                P(sp, "tp"),
                P(None, "tp", sp),
                P(None, "tp"),
                P(None, "tp", sp),
                P(None, "tp", sp),
                P(),
                P(None, "tp"),
                P(),
                P(sp, "tp"),
                P(sp, "tp"),
                P(None, "tp"),
                P("tp", sp),
            ),
            out_specs=P(sp, "tp"),
            check_vma=False,
        )(*args)

    return layer
```

```python
import functools
import jax
import jax.numpy as jnp
from jax import lax
from jax.experimental import pallas as pl
from jax.experimental.pallas import tpu as pltpu
from jax.sharding import Mesh, PartitionSpec as P

DK = 128
EPS = 1e-06
F32 = jnp.float32
BF16 = jnp.bfloat16


def halves(x):
    high = x.astype(BF16)
    return high, (x - high.astype(F32)).astype(BF16)


def contract(a, b, da, db):
    return lax.dot_general(a, b, (((da,), (db,)), ((), ())), preferred_element_type=F32)


def dot_halves(a, b):
    ah, al = a
    bh, bl = b
    return contract(ah, bh, 1, 0) + (contract(ah, bl, 1, 0) + contract(al, bh, 1, 0))


def dot(a, b):
    return dot_halves(halves(a), halves(b))


def dot_nt(a, b):
    return contract(a, b, 1, 1)


def inverses_unit_triangular(stricts, row, col):
    width = stricts[0].shape[0]
    identity = (row == col).astype(F32)
    apart = (row // 2 == col // 2) & (row != col)
    found = [identity - jnp.where(apart, strict, 0.0) for strict in stricts]
    size = 2
    while size < width:
        apart = (row // (2 * size) == col // (2 * size)) & (row // size != col // size)
        split = [halves(item) for item in found]
        offs = [halves(jnp.where(apart, strict, 0.0)) for strict in stricts]
        inner = [halves(dot_halves(off, item)) for off, item in zip(offs, split)]
        steps = [dot_halves(item, part) for item, part in zip(split, inner)]
        found = [item - step for item, step in zip(found, steps)]
        size *= 2
    return found


def delta_kernel(tokens_ref, reach_ref, own_ref, maps_ref, *, width, rows):
    blocks = tokens_ref.shape[0]
    per = rows // width
    count = blocks * per
    row = lax.broadcasted_iota(jnp.int32, (width, width), 0)
    col = lax.broadcasted_iota(jnp.int32, (width, width), 1)
    eye = row == col
    identity = eye.astype(F32)
    stricts, rights, readers, carriers, grown_queries, ends = [], [], [], [], [], []
    for n in range(count):
        block, part = divmod(n, per)
        at = slice(part * width, (part + 1) * width)
        q = tokens_ref[block, at, 0:DK]
        k = tokens_ref[block, at, DK : 2 * DK]
        v = tokens_ref[block, at, 2 * DK : 3 * DK].astype(F32)
        qf = q.astype(F32)
        kf = k.astype(F32)
        kk = dot_nt(k, k)
        qk = dot_nt(q, k)
        diagonal = jnp.where(eye, kk, 0.0)
        key_col = lax.rsqrt(jnp.sum(kf * kf, axis=1, keepdims=True) + EPS)
        key_row = lax.rsqrt(jnp.sum(diagonal, axis=0, keepdims=True) + EPS)
        query_col = lax.rsqrt(jnp.sum(qf * qf, axis=1, keepdims=True) + EPS) * DK ** (-0.5)
        kk = kk * key_col * key_row
        qk = qk * query_col * key_row
        keys = kf * key_col
        queries = qf * query_col
        bits = tokens_ref[block, rows : rows + 16, :].astype(F32)
        joined = bits[0:1] + (bits[1:2] + bits[2:3])
        lines = [joined[:, i * rows + part * width : i * rows + (part + 1) * width] for i in range(4)]
        across = jnp.concatenate(lines + [jnp.zeros((4, width), F32)], axis=0)
        down = jnp.transpose(across)
        for d in range(2):
            inside = (col <= row) if d == 0 else (col >= row)
            sooner = (row <= col) if d == 0 else (row >= col)
            ld_row = across[d : d + 1]
            ld_col = down[:, d : d + 1]
            beta = down[:, 2 + d : 3 + d]
            cum_col = jnp.sum(jnp.where(inside, ld_row, 0.0), axis=1, keepdims=True)
            cum_row = jnp.sum(jnp.where(sooner, ld_col, 0.0), axis=0, keepdims=True)
            total = jnp.sum(ld_row, axis=1, keepdims=True)
            decay = jnp.exp(jnp.where(inside, cum_col - cum_row, -1e30))
            stricts.append(jnp.where(eye, 0.0, kk * decay * beta))
            grown = jnp.exp(cum_col)
            rights.append(jnp.concatenate([keys * (beta * grown), v * beta], axis=1))
            readers.append(qk * decay)
            carriers.append(jnp.transpose(keys * jnp.exp(total - cum_col)))
            grown_queries.append(queries * grown)
            ends.append(jnp.exp(total))
    found = inverses_unit_triangular(stricts, row, col)
    solved = [halves(dot(item, right)) for item, right in zip(found, rights)]
    both = [
        dot_halves(halves(jnp.concatenate([reader, carrier], axis=0)), item)
        for reader, carrier, item in zip(readers, carriers, solved)
    ]
    own = [None] * count
    states = [None, None]
    for step in range(count):
        for d in range(2):
            n = step if d == 0 else count - 1 - step
            i = 2 * n + d
            reach = grown_queries[i] - both[i][:width, :DK]
            local = both[i][:width, DK:]
            transition = identity * ends[i] - both[i][width:, :DK]
            addition = both[i][width:, DK:]
            if states[d] is None:
                states[d] = jnp.concatenate([transition, addition], axis=1)
            else:
                moved = dot(jnp.concatenate([reach, transition], axis=0), states[d])
                reach = moved[:width, :DK]
                local = local + moved[:width, DK:]
                states[d] = moved[width:] + jnp.concatenate(
                    [jnp.zeros_like(addition), addition], axis=1
                )
            reach_ref[d, n * width : (n + 1) * width] = reach
            own[n] = local if own[n] is None else own[n] + local
    maps_ref[0] = states[0]
    maps_ref[1] = states[1]
    for n in range(count):
        own_ref[n * width : (n + 1) * width] = own[n]


def finish_kernel(place_ref, maps_ref, reach_ref, own_ref, valve_ref, gain_ref, mixed_ref):
    z = place_ref[0]
    planes = maps_ref.shape[0]
    empty = jnp.zeros((DK, own_ref.shape[1]), F32)

    def absorb(at, state):
        item = maps_ref[at]
        return dot(item[:, :DK], state) + item[:, DK:]

    ahead = lax.fori_loop(0, z, absorb, empty)
    behind = lax.fori_loop(
        0, planes - 1 - z, lambda i, state: absorb(planes - 1 - i, state), empty
    )
    o = own_ref[...] + dot(reach_ref[0], ahead) + dot(reach_ref[1], behind)
    scaled = o * lax.rsqrt(jnp.mean(o * o, axis=1, keepdims=True) + EPS) * gain_ref[...]
    copies, blocks, rows, _ = mixed_ref.shape
    valve = jnp.concatenate(
        [valve_ref[j, :rows, 3 * DK :].astype(F32) for j in range(blocks)], axis=0
    )
    mixed = (scaled * (valve / (1.0 + jnp.exp(-valve)))).astype(BF16)
    for i in range(copies):
        for j in range(blocks):
            mixed_ref[i, j] = mixed[j * rows : (j + 1) * rows]


def vmem(count):
    return [pl.BlockSpec(memory_space=pltpu.VMEM)] * count


def delta_rule(tokens, rows):
    length = tokens.shape[0] * rows
    width = min(128, rows)
    return pl.pallas_call(
        functools.partial(delta_kernel, width=width, rows=rows),
        out_shape=(
            jax.ShapeDtypeStruct((2, length, DK), F32),
            jax.ShapeDtypeStruct((length, DK), F32),
            jax.ShapeDtypeStruct((2, DK, 2 * DK), F32),
        ),
        in_specs=vmem(1),
        out_specs=tuple(vmem(3)),
        name="delta_rule",
    )(tokens)


def pack_kernel(q_ref, k_ref, v_ref, gate_ref, shrink_ref, speed_ref, insertion_ref, spike_ref, out_ref):
    group, _, _ = out_ref.shape
    rows = q_ref.shape[0]
    for j in range(group):
        for i, ref in enumerate((q_ref, k_ref, v_ref, gate_ref)):
            out_ref[j, :rows, span(i, DK)] = ref[:, span(j, DK)]
        lines = []
        for d in range(2):
            raw = shrink_ref[d, j : j + 1]
            soft = jnp.maximum(raw, 0.0) + jnp.log1p(jnp.exp(-jnp.abs(raw)))
            lines.append(spike_ref[d, j : j + 1] - speed_ref[d, j] * soft)
        for d in range(2):
            lines.append(1.0 / (1.0 + jnp.exp(-insertion_ref[d, j : j + 1])))
        line = jnp.concatenate(lines, axis=1)
        high, rest = halves(line)
        middle = rest
        low = (line - high.astype(F32) - middle.astype(F32)).astype(BF16)
        bits = [high.astype(F32), middle.astype(F32), low.astype(F32)]
        bits.append(jnp.zeros((13, 4 * rows), F32))
        out_ref[j, rows:] = jnp.concatenate(bits, axis=0).astype(BF16)


def pack_tokens(q, k, v, gate, shrink, speed, insertion, spike):
    rows = q.shape[0]
    group = q.shape[1] // DK
    specs = vmem(5) + [pl.BlockSpec(memory_space=pltpu.SMEM)] + vmem(2)
    return pl.pallas_call(
        pack_kernel,
        out_shape=jax.ShapeDtypeStruct((group, rows + 16, 4 * DK), BF16),
        in_specs=specs,
        out_specs=pl.BlockSpec(memory_space=pltpu.VMEM),
        name="pack_tokens",
    )(q, k, v, gate, shrink, speed, insertion, spike)


def finish(place, maps, reach, own, valve, gain, group):
    rows = own.shape[0] // group
    return pl.pallas_call(
        finish_kernel,
        out_shape=jax.ShapeDtypeStruct((group, group, rows, DK), BF16),
        in_specs=[pl.BlockSpec(memory_space=pltpu.SMEM)] + vmem(5),
        out_specs=pl.BlockSpec(memory_space=pltpu.VMEM),
        name="finish",
    )(place, maps, reach, own, valve, gain)


def copy_kernel(*refs, moves, sources):
    output = refs[sources]
    for source, take, put in moves:
        output[put] = refs[source][take]


def rearrange(arrays, shape, moves, name):
    count = len(arrays)
    return pl.pallas_call(
        functools.partial(copy_kernel, moves=tuple(moves), sources=count),
        out_shape=jax.ShapeDtypeStruct(shape, arrays[0].dtype),
        in_specs=vmem(count),
        out_specs=pl.BlockSpec(memory_space=pltpu.VMEM),
        name=name,
    )(*arrays)


def span(index, size):
    return pl.ds(index * size, size)


ALL = slice(None)


def send_kernel(place_ref, *refs, late):
    outs = refs[2 if late else 1 :]
    group = len(outs)
    for r in range(group):
        to = (place_ref[0] + r) % group
        units = outs[r].shape[-1]
        at = pl.ds(pl.multiple_of(to * units, units), units)
        if late:
            outs[r][0] = refs[0][:, at]
            outs[r][1] = jnp.transpose(refs[1][at].astype(F32)).astype(BF16)
        else:
            outs[r][...] = refs[0][:, at]


def pack_sends(place, arrays, group, name):
    depth = arrays[0].shape[0]
    units = arrays[0].shape[1] // group
    late = len(arrays) == 2
    shape = (2, depth, units) if late else (depth, units)
    return pl.pallas_call(
        functools.partial(send_kernel, late=late),
        out_shape=[jax.ShapeDtypeStruct(shape, BF16)] * group,
        in_specs=[pl.BlockSpec(memory_space=pltpu.SMEM)] + vmem(len(arrays)),
        out_specs=vmem(group),
        name=name,
    )(place, *arrays)


def rotate(pieces, axis):
    group = len(pieces)
    return [pieces[0]] + [
        lax.ppermute(pieces[r], axis, [(i, (i + r) % group) for i in range(group)])
        for r in range(1, group)
    ]


def place_kernel(place_ref, *refs):
    out_ref = refs[-1]
    group = len(refs) - 1
    for r in range(group):
        source = lax.rem(place_ref[0] + group - r, group)
        if out_ref.ndim == 4:
            for w in range(out_ref.shape[0]):
                out_ref[w, source] = refs[r][w]
        else:
            out_ref[source] = refs[r][...]


def place_pieces(place, pieces, name):
    group = len(pieces)
    shape = pieces[0].shape
    shape = shape[:-2] + (group,) + shape[-2:]
    return pl.pallas_call(
        place_kernel,
        out_shape=jax.ShapeDtypeStruct(shape, BF16),
        in_specs=[pl.BlockSpec(memory_space=pltpu.SMEM)] + vmem(group),
        out_specs=pl.BlockSpec(memory_space=pltpu.VMEM),
        name=name,
    )(place, *pieces)


def down_kernel(hidden_ref, weight_ref, out_ref):
    tile = out_ref.shape[2]
    product = contract(hidden_ref[...], weight_ref[0], 1, 1).astype(BF16)
    for c in range(out_ref.shape[0]):
        out_ref[c] = product[:, span(c, tile)]


def down_product(hidden, weight, cores, places):
    length, units = hidden.shape
    features = weight.shape[1] // cores
    tile = features // places
    return pl.pallas_call(
        down_kernel,
        grid=(places,),
        out_shape=jax.ShapeDtypeStruct((cores, length, features), BF16),
        in_specs=[
            pl.BlockSpec((length, units), lambda n: (0, 0)),
            pl.BlockSpec((1, cores * tile, units), lambda n: (1, n, 0)),
        ],
        out_specs=pl.BlockSpec((cores, length, tile), lambda n: (0, 0, n)),
        name="down",
    )(hidden, weight)


def norm_kernel(rows_ref, gain_ref, out_ref, *, sets, places):
    cores, _, features = rows_ref.shape
    parts = [rows_ref[c].astype(F32) for c in range(cores)]
    total = sum(jnp.sum(part * part, axis=1, keepdims=True) for part in parts)
    scale = lax.rsqrt(total / (cores * features) + EPS)
    wide = cores * features // (sets * places)
    each = features // wide
    for c in range(cores):
        scaled = (parts[c] * scale * gain_ref[:, span(c, features)]).astype(BF16)
        for j in range(each):
            set_at, place = divmod(c * each + j, places)
            at = place * sets + set_at
            out_ref[:, span(at, wide)] = scaled[:, span(j, wide)]


def norm_rows(rows, gain, sets, places):
    cores, length, features = rows.shape
    tile = min(128, length)
    return pl.pallas_call(
        functools.partial(norm_kernel, sets=sets, places=places),
        grid=(length // tile,),
        out_shape=jax.ShapeDtypeStruct((length, cores * features), BF16),
        in_specs=[
            pl.BlockSpec((cores, tile, features), lambda i: (0, i, 0)),
            pl.BlockSpec((1, cores * features), lambda i: (0, 0)),
        ],
        out_specs=pl.BlockSpec((tile, cores * features), lambda i: (i, 0)),
        name="norm_rows",
    )(rows, gain)


def project_kernel(place_ref, parcels_ref, weight_ref, *refs):
    skips, out_ref, heads_ref = refs[:-2], refs[-2], refs[-1]
    cores, sets, group, rows, size = parcels_ref.shape
    for r in range(sets):
        source = lax.rem(place_ref[0] + sets - r, sets)
        for c in range(cores):
            for j in range(group):
                heads_ref[r * rows : (r + 1) * rows, span(c * group + j, size)] = parcels_ref[
                    c, source, j
                ]
    projected = jnp.dot(heads_ref[...], weight_ref[...], preferred_element_type=F32)
    for r in range(sets):
        source = lax.rem(place_ref[0] + sets - r, sets)
        total = skips[r][...].astype(F32) + projected[r * rows : (r + 1) * rows]
        out_ref[pl.ds(source * rows, rows)] = total.astype(BF16)


def project(place, parcels, weight, skips):
    cores, sets, group, rows, size = parcels.shape
    features = weight.shape[1]
    return pl.pallas_call(
        project_kernel,
        out_shape=jax.ShapeDtypeStruct((sets * rows, features), BF16),
        in_specs=[pl.BlockSpec(memory_space=pltpu.SMEM)] + vmem(2 + sets),
        out_specs=pl.BlockSpec(memory_space=pltpu.VMEM),
        scratch_shapes=[pltpu.VMEM((sets * rows, cores * group * size), BF16)],
        name="project",
    )(place, parcels, weight, *skips)


def add_kernel(parts_ref, out_ref):
    total = parts_ref[0].astype(F32)
    for c in range(1, parts_ref.shape[0]):
        total = total + parts_ref[c].astype(F32)
    out_ref[...] = total.astype(BF16)


def add_cores(parts):
    cores, length, features = parts.shape
    tile = min(128, length)
    return pl.pallas_call(
        add_kernel,
        grid=(length // tile,),
        out_shape=jax.ShapeDtypeStruct((length, features), BF16),
        in_specs=[pl.BlockSpec((cores, tile, features), lambda i: (0, i, 0))],
        out_specs=pl.BlockSpec((tile, features), lambda i: (i, 0)),
        name="add_cores",
    )(parts)


def result_kernel(parts_ref, middle_ref, out_ref, *, sets, wide):
    total = parts_ref[0].astype(F32)
    for i in range(1, parts_ref.shape[0]):
        total = total + parts_ref[i].astype(F32)
    places = total.shape[1] // (sets * wide)
    for i in range(sets):
        for j in range(places):
            at = span(i * places + j, wide)
            from_at = j * sets + i
            added = middle_ref[:, at].astype(F32) + total[:, from_at * wide : (from_at + 1) * wide]
            out_ref[:, at] = added.astype(BF16)


def add_result(parts, middle, sets, wide):
    return pl.pallas_call(
        functools.partial(result_kernel, sets=sets, wide=wide),
        out_shape=jax.ShapeDtypeStruct(middle.shape, BF16),
        in_specs=vmem(2),
        out_specs=pl.BlockSpec(memory_space=pltpu.VMEM),
        name="add_result",
    )(parts, middle)


def after(value, other):
    return lax.optimization_barrier((value, other))[0]


def exchange(slots, axis):
    return lax.all_to_all(slots, axis, split_axis=0, concat_axis=0, tiled=True)


def to_columns(stack):
    return jnp.transpose(stack, (1, 0, 2)).reshape(stack.shape[1], -1)


def body(
    skip_pathway,
    request_vectors,
    lookup_address_matrix,
    content_vectors,
    result_valve_matrix,
    shrink_raw_signal,
    channel_shrink_speed,
    insertion_raw_signal,
    extra_shrink_spike,
    channel_scaling_vector,
    final_mapping_matrix,
    mixer_scaling_vector,
    valve_matrix,
    widening_matrix,
    temporal_kernel_entries,
    narrowing_matrix,
):
    group = lax.axis_size("p")
    chain = ("a", "m")
    ring = ("m", "p")
    planes = lax.axis_size("a") * lax.axis_size("m")
    places = lax.axis_size("m") * group
    cores = lax.axis_size("tp")
    a = lax.axis_index("a")
    z = a * lax.axis_size("m") + lax.axis_index("m")
    place = lax.axis_index("m") * group + lax.axis_index("p")
    rows, features = skip_pathway.shape
    length = group * rows
    depth, hidden_size = valve_matrix.shape
    units = hidden_size // group

    here = a.reshape(1).astype(jnp.int32)
    packed = pack_tokens(
        request_vectors,
        lookup_address_matrix,
        content_vectors,
        result_valve_matrix,
        shrink_raw_signal,
        channel_shrink_speed,
        insertion_raw_signal,
        extra_shrink_spike,
    )
    tokens = exchange(packed, "p")
    first = rotate(pack_sends(here, (valve_matrix,), group, "pack_valve"), "a")
    skips = rotate([skip_pathway] * group, "a")
    if narrowing_matrix.shape[1] == depth and depth % 128 == 0:
        late = pack_sends(here, (widening_matrix, narrowing_matrix), group, "pack_late")
    else:
        both = jnp.stack([widening_matrix, jnp.transpose(narrowing_matrix)])
        late = [
            lax.dynamic_slice_in_dim(both, (a + r) % group * units, units, axis=2)
            for r in range(group)
        ]

    reach, own, maps = delta_rule(tokens, rows)
    *first, reach = lax.optimization_barrier((*first, reach))
    first = place_pieces(here, first, "place_valve").reshape(group * depth, units)
    valve_full = lax.all_gather(first, ring, axis=0, tiled=True)
    *late, _ = lax.optimization_barrier((*late, first))
    late = rotate(late, "a")
    plane_ids = jnp.arange(planes).reshape(planes, 1, 1)
    outgoing = jnp.where(plane_ids > z, maps[0][None], maps[1][None])
    incoming = exchange(outgoing, chain)
    mixed = finish(
        z.reshape(1).astype(jnp.int32),
        incoming,
        reach,
        own,
        tokens,
        channel_scaling_vector.reshape(1, -1),
        group,
    )

    *late, mixed = lax.optimization_barrier((*late, mixed))
    late = place_pieces(here, late, "place_late").reshape(2, group * depth, units)
    late = lax.all_gather(late, ring, axis=1, tiled=True)

    heads = exchange(mixed.reshape(group * group, rows, DK), ("a", "p"))
    heads = exchange(jnp.broadcast_to(heads[None], (cores,) + heads.shape), "tp")
    heads = heads.reshape(cores, group, group, rows, DK)
    middle = project(here, heads, final_mapping_matrix, skips)
    full_rows = exchange(jnp.broadcast_to(middle[None], (cores,) + middle.shape), "tp")
    normed = norm_rows(full_rows, mixer_scaling_vector.reshape(1, -1), group, places)

    gate = jnp.dot(normed, valve_full, preferred_element_type=F32).astype(BF16)
    gate = gate.reshape(group, rows, units)
    up = jnp.dot(normed, late[0], preferred_element_type=F32)
    blank = jnp.zeros((1, 1, units), BF16)
    before = lax.ppermute(gate[:, -1:], ring, [(i, (i + 1) % places) for i in range(places)])
    later = lax.ppermute(gate[:, :1], ring, [((i + 1) % places, i) for i in range(places)])
    before = jnp.where(place == 0, jnp.concatenate([blank, before[:-1]]), before)
    later = jnp.where(place == places - 1, jnp.concatenate([later[1:], blank]), later)
    padded = jnp.concatenate([before, gate, later], axis=1).astype(F32)
    taps = lax.dynamic_slice_in_dim(temporal_kernel_entries, a * units, units, axis=1)
    convolved = padded[:, :-2] * taps[0] + padded[:, 1:-1] * taps[1] + padded[:, 2:] * taps[2]
    hidden = (jax.nn.silu(convolved.reshape(length, units)) * up).astype(BF16)
    mine = lax.dynamic_slice_in_dim(middle, a * rows, rows, axis=0)
    wide = cores * features // (group * places)
    aligned = group % cores == 0 and features // places % 128 == 0
    if aligned:
        terms = down_product(hidden, late, cores, places)
    else:
        natural = late[1].reshape(places, group, wide, units)
        natural = jnp.transpose(natural, (1, 0, 2, 3)).reshape(cores, features, units)
        terms = jnp.einsum("tk,cfk->ctf", hidden, natural, preferred_element_type=F32)
        terms = terms.astype(BF16)
    terms = add_cores(exchange(terms, "tp"))
    terms = exchange(terms.reshape(group, rows, features), "a")
    if aligned:
        return add_result(terms, mine, group // cores, wide)
    return (mine.astype(F32) + jnp.sum(terms.astype(F32), axis=0)).astype(BF16)


def solution(mesh):
    def layer(*args):
        cores = mesh.shape["tp"]
        group = args[5].shape[1] // cores
        split = Mesh(mesh.devices.reshape(group, -1, group, cores), ("a", "m", "p", "tp"))
        sp = ("a", "m", "p")
        return jax.shard_map(
            body,
            mesh=split,
            in_specs=(
                P(sp, "tp"),
                P(sp, "tp"),
                P(sp, "tp"),
                P(sp, "tp"),
                P(sp, "tp"),
                P(None, "tp", sp),
                P(None, "tp"),
                P(None, "tp", sp),
                P(None, "tp", sp),
                P(),
                P(None, "tp"),
                P(),
                P(sp, "tp"),
                P(sp, "tp"),
                P(None, "tp"),
                P("tp", sp),
            ),
            out_specs=P(sp, "tp"),
            check_vma=False,
        )(*args)

    return layer
```
